32 devices in a mesh: sp: 8 (over z, x), tp: 4 (over y, core).
Axes of the slice: x: 2, y: 2, z: 4, core: 2. Of those that a mesh axis runs over, the one named last changes fastest.
Arguments:
- inputs: bfloat16 [8192, 2048], P('sp'), may hold values from -9 to 9
- w_query: bfloat16 [2048, 1024], P(None, 'tp'), may hold values from -0.15692044 to 0.15692044
- w_key: bfloat16 [2048, 1024], P(None, 'tp'), may hold values from -0.15692044 to 0.15692044
- w_value: bfloat16 [2048, 1024], P(None, 'tp'), may hold values from -0.125 to 0.125
- w_glu_value: bfloat16 [2048, 1024], P(None, 'tp'), may hold values from -0.37565048 to 0.37565048
- w_glu_gate: bfloat16 [2048, 1024], P(None, 'tp'), may hold values from -0.125 to 0.125
- conv_taps: float32 [31, 1024], P(None, 'tp'), may hold values from -4 to 4
- conv_gain: float32 [1024], P('tp'), may hold values from 0.1 to 1.9
- log_forget: float32 [8192, 8], P('sp', 'tp'), may hold values from -8192 to 0, as said below
- w_out: bfloat16 [2048, 2048], replicated, may hold values from -0.125 to 0.125
Outputs:
- result: bfloat16 [8192, 2048], P(('sp', 'tp'))
The draws below stay inside these ranges and needn't reach their ends.
Inputs may be any that keep to these rules, and one draw needn't show every extreme that they name: `log_forget`: for each head, non-increasing along positions and at most zero.
All inputs are finite; a program needn't handle non-finite values.
Results may differ from the reference program's by a relative error of at most 0.014.
Values may be sent and summed in bfloat16 or wider, within the bound.
A program may use at most 128 MiB of HBM per device.

```python
import jax
import jax.numpy as jnp
from jax import lax

D_MODEL = 2048
HEADS = 8
HEAD_DIM = 128
CONV_CH = 1024
KERNEL = 31
TOK_DEV = 1024
SEQUENCE_TOKENS = 8192


def draw_inputs(key, part):
    values = jnp.clip(jax.random.normal(jax.random.fold_in(key, 1), (SEQUENCE_TOKENS, D_MODEL), jnp.float32), -4.0, 4.0)
    return values.astype(jnp.bfloat16)


def weight_spread():
    return (3.0 / D_MODEL) ** 0.5


def query_base(key):
    return jax.random.normal(jax.random.fold_in(key, 11), (D_MODEL, HEADS * HEAD_DIM), jnp.float32) * weight_spread()


def draw_w_query(key, part):
    bound = 4.0 * weight_spread()
    return jnp.clip(query_base(key), -bound, bound).astype(jnp.bfloat16)


def draw_w_key(key, part):
    bound = 4.0 * weight_spread()
    other = jax.random.normal(jax.random.fold_in(key, 12), (D_MODEL, HEADS * HEAD_DIM), jnp.float32) * weight_spread()
    return jnp.clip(other, -bound, bound).astype(jnp.bfloat16)


def draw_w_glu_value(key, part):
    ramp = jnp.arange(CONV_CH, dtype=jnp.float32) / max(CONV_CH - 1, 1)
    shared_scale = 10.0 ** (ramp - 0.5)
    own_part = jnp.clip(jax.random.normal(jax.random.fold_in(key, 41), (D_MODEL, CONV_CH), jnp.float32), -4.0, 4.0)
    shared_column = jnp.clip(jax.random.normal(jax.random.fold_in(key, 42), (D_MODEL, 1), jnp.float32), -4.0, 4.0)
    values = (own_part + shared_scale[None, :] * shared_column) * D_MODEL ** (-0.5)
    return values.astype(jnp.bfloat16)


def draw_conv_taps(key, part):
    ramp = jnp.arange(CONV_CH, dtype=jnp.float32) / max(CONV_CH - 1, 1)
    raw = jnp.clip(jax.random.normal(jax.random.fold_in(key, 21), (KERNEL, CONV_CH), jnp.float32), -5.0, 5.0)
    scales = 10.0 ** (0.8 * ramp - 0.4)
    return (raw + 1.0) * scales[None, :] * KERNEL ** (-0.5)


def draw_log_forget(key, part):
    ranks = jax.random.permutation(jax.random.fold_in(key, 31), HEADS)
    fast_count = HEADS // 2
    is_fast = ranks < fast_count
    fast_rate = 1.0 / jax.random.uniform(jax.random.fold_in(key, 32), (HEADS,), jnp.float32, 30.0, 100.0)
    slow_total = jnp.exp(jax.random.uniform(jax.random.fold_in(key, 33), (HEADS,), jnp.float32, jnp.log(0.3), jnp.log(1.0)))
    decay_rate = jnp.where(is_fast, fast_rate, slow_total / SEQUENCE_TOKENS)
    block_count = SEQUENCE_TOKENS // TOK_DEV
    block_multiplier = jnp.exp(jax.random.uniform(jax.random.fold_in(key, 34), (block_count,), jnp.float32, jnp.log(0.5), jnp.log(2.0)))
    block_multiplier = jnp.repeat(block_multiplier, TOK_DEV)
    coarse_estimate = jax.random.uniform(jax.random.fold_in(key, 35), (SEQUENCE_TOKENS, HEADS), jnp.float32, 0.2, 1.8)
    spike_position = jax.random.randint(jax.random.fold_in(key, 36), (3,), 0, SEQUENCE_TOKENS)
    spike_loss = jax.random.uniform(jax.random.fold_in(key, 37), (3,), jnp.float32, 0.2, 0.4)
    spike_list = jnp.zeros((SEQUENCE_TOKENS,), jnp.float32).at[spike_position].add(jnp.log(1.0 - spike_loss))
    step_count = -decay_rate[None, :] * coarse_estimate * block_multiplier[:, None] + spike_list[:, None]
    return jnp.cumsum(step_count, axis=0)


def block_levels(stream_key, dims, pieces, smallest, high):
    factor_of = 1.0
    for position, shards_of in pieces:
        draws = jax.random.uniform(jax.random.fold_in(jax.random.fold_in(stream_key, 6), position), (shards_of,), jnp.float32, smallest / len(pieces), high / len(pieces))
        factor_of = factor_of * jnp.repeat(jnp.exp(draws), dims[position] // shards_of).reshape((-1,) + (1,) * (len(dims) - 1 - position))
    return factor_of


def noise(stream_key, dims, deviation, reach, pieces=(), kind=jnp.bfloat16):
    drawn = deviation * jax.random.normal(stream_key, dims, jnp.float32)
    if pieces:
        drawn = drawn * block_levels(stream_key, dims, pieces, -0.22, 0.18)
    return jnp.clip(drawn, -reach, reach).astype(kind)


def setup_inputs(seed: int = 0) -> dict:
    arg_keys = jax.random.split(jax.random.key(seed), 11)
    inputs = draw_inputs(jax.random.fold_in(arg_keys[10], 71), 0)
    w_query = draw_w_query(jax.random.fold_in(arg_keys[10], 71), 0)
    w_key = draw_w_key(jax.random.fold_in(arg_keys[10], 71), 0)
    w_value = noise(arg_keys[3], (D_MODEL, HEADS * HEAD_DIM), D_MODEL ** -0.5, 0.125, ((1, 4),))
    w_glu_value = draw_w_glu_value(jax.random.fold_in(arg_keys[10], 71), 0)
    w_glu_gate = noise(arg_keys[5], (D_MODEL, CONV_CH), D_MODEL ** -0.5, 0.125, ((1, 4),))
    conv_taps = draw_conv_taps(jax.random.fold_in(arg_keys[10], 71), 0)
    conv_gain = jnp.clip(1.0 + 0.18 * jax.random.normal(arg_keys[7], (CONV_CH,), jnp.float32), 0.1, 1.9)
    log_forget = draw_log_forget(jax.random.fold_in(arg_keys[10], 71), 0)
    w_out = noise(arg_keys[9], (CONV_CH + HEADS * HEAD_DIM, D_MODEL), (CONV_CH + HEADS * HEAD_DIM) ** -0.5, 0.125)
    return dict(inputs=inputs, w_query=w_query, w_key=w_key, w_value=w_value, w_glu_value=w_glu_value, w_glu_gate=w_glu_gate, conv_taps=conv_taps, conv_gain=conv_gain, log_forget=log_forget, w_out=w_out)


NORM_EPS = 1e-05

def reference(inputs, w_query, w_key, w_value, w_glu_value, w_glu_gate, conv_taps, conv_gain, log_forget, w_out):
    glu_value = jnp.dot(inputs, w_glu_value, preferred_element_type=jnp.float32)
    glu_gate = jnp.dot(inputs, w_glu_gate, preferred_element_type=jnp.float32)
    gated = (glu_value * jax.nn.sigmoid(glu_gate)).astype(jnp.bfloat16)
    padded = jnp.concatenate([jnp.zeros((KERNEL - 1, CONV_CH), jnp.bfloat16), gated], axis=0).astype(jnp.float32)
    conv_sum = jnp.zeros((SEQUENCE_TOKENS, CONV_CH), jnp.float32)
    for offset in range(KERNEL):
        conv_sum = conv_sum + conv_taps[offset] * padded[offset:offset + SEQUENCE_TOKENS]
    mean_value = lax.optimization_barrier(jnp.mean(conv_sum, axis=1, keepdims=True))
    centered = conv_sum - mean_value
    spread = lax.optimization_barrier(jnp.mean(centered * centered, axis=1, keepdims=True))
    conv_rows = jax.nn.silu(centered * lax.rsqrt(spread + NORM_EPS) * conv_gain).astype(jnp.bfloat16)
    query_rows = jnp.dot(inputs, w_query, preferred_element_type=jnp.float32).astype(jnp.bfloat16)
    key_rows = jnp.dot(inputs, w_key, preferred_element_type=jnp.float32).astype(jnp.bfloat16)
    value_rows = jnp.dot(inputs, w_value, preferred_element_type=jnp.float32).astype(jnp.bfloat16)
    blocks = SEQUENCE_TOKENS // TOK_DEV
    query_heads = query_rows.reshape(SEQUENCE_TOKENS, HEADS, HEAD_DIM).transpose(1, 0, 2).reshape(HEADS, blocks, TOK_DEV, HEAD_DIM)
    key_heads = key_rows.reshape(SEQUENCE_TOKENS, HEADS, HEAD_DIM).transpose(1, 0, 2)
    value_heads = value_rows.reshape(SEQUENCE_TOKENS, HEADS, HEAD_DIM).transpose(1, 0, 2)
    gate_heads = jnp.transpose(log_forget)
    gate_blocks = gate_heads.reshape(HEADS, blocks, TOK_DEV)
    positions = jnp.arange(SEQUENCE_TOKENS, dtype=jnp.int32)
    block_starts = jnp.arange(blocks, dtype=jnp.int32) * TOK_DEV
    score_scale = HEAD_DIM ** (-0.5)

    def head_output(packed):
        head_query, head_key, head_value, head_gate, head_gate_blocks = packed

        def block_output(block_packed):
            block_query, block_gate, block_start = block_packed
            scores = jnp.dot(block_query, head_key.T, preferred_element_type=jnp.float32) * score_scale
            scores = scores + block_gate[:, None] - head_gate[None, :]
            query_pos = block_start + jnp.arange(TOK_DEV, dtype=jnp.int32)
            allowed = positions[None, :] <= query_pos[:, None]
            scores = jnp.where(allowed, scores, -jnp.inf)
            row_max = lax.optimization_barrier(jnp.max(scores, axis=1, keepdims=True))
            weights = jnp.exp(scores - row_max)
            denominators = lax.optimization_barrier(jnp.sum(weights, axis=1, keepdims=True))
            mixture = jnp.dot(weights.astype(jnp.bfloat16), head_value, preferred_element_type=jnp.float32)
            return (mixture / denominators).astype(jnp.bfloat16)
        return lax.map(block_output, (head_query, head_gate_blocks, block_starts))
    attn_heads = lax.map(head_output, (query_heads, key_heads, value_heads, gate_heads, gate_blocks))
    attn_rows = attn_heads.reshape(HEADS, SEQUENCE_TOKENS, HEAD_DIM).transpose(1, 0, 2).reshape(SEQUENCE_TOKENS, HEADS * HEAD_DIM)
    projected = jnp.dot(conv_rows, w_out[:CONV_CH], preferred_element_type=jnp.float32)
    projected = projected + jnp.dot(attn_rows, w_out[CONV_CH:], preferred_element_type=jnp.float32)
    return projected.astype(jnp.bfloat16)
```

```python
import functools

import jax
import jax.numpy as jnp
from jax import lax
from jax.experimental import pallas as pl
from jax.experimental.pallas import tpu as pltpu
from jax.sharding import PartitionSpec as P

HEAD_DIM = 128
NORM_EPS = 1e-05
LOG2E = 1.4426950408889634
GATE_PARTS = 3


def split_gates(gates):
    high = lax.reduce_precision(gates, 8, 7)
    middle = lax.reduce_precision(gates - high, 8, 7)
    low = gates - high - middle
    return jnp.stack([high, middle, low]).astype(jnp.bfloat16)


def flash_body(
    info_ref, q_ref, fq_ref, kv_ref, *refs, heads, rows, causal, first, last, gate_rows
):
    if first:
        outs = refs
    else:
        acc_in, max_in, sum_in = refs[:3]
        outs = refs[3:]
    width = heads * HEAD_DIM
    tile = q_ref.shape[0]
    q_first = info_ref[0] + lax.rem(pl.program_id(0) * tile, rows)
    q_first = jnp.where(pl.program_id(0) * tile >= rows, q_first + info_ref[1], q_first)
    key_first = info_ref[2]
    lanes = kv_ref.shape[1]

    def step(old):
        for h in range(heads):
            columns = slice(h * HEAD_DIM, (h + 1) * HEAD_DIM)
            keys = kv_ref[:rows, columns]
            values = kv_ref[:rows, width + h * HEAD_DIM : width + (h + 1) * HEAD_DIM]
            base = rows + h * GATE_PARTS * gate_rows
            packed = kv_ref[base : base + GATE_PARTS * gate_rows, :].astype(jnp.float32)
            pieces = []
            for g in range(gate_rows):
                total = packed[g : g + 1]
                for part in range(1, GATE_PARTS):
                    total = total + packed[part * gate_rows + g : part * gate_rows + g + 1]
                pieces.append(total)
            gates = jnp.concatenate(pieces, axis=1)
            bias = (fq_ref[h : h + 1, 0:1] - gates) * LOG2E
            scores = lax.dot_general(
                q_ref[:, columns],
                keys,
                (((1,), (1,)), ((), ())),
                preferred_element_type=jnp.float32,
            )
            scores = scores * (HEAD_DIM ** (-0.5) * LOG2E) + bias
            if causal:
                row_pos = q_first + lax.broadcasted_iota(jnp.int32, scores.shape, 0)
                key_pos = key_first + lax.broadcasted_iota(jnp.int32, scores.shape, 1)
                scores = jnp.where(key_pos <= row_pos, scores, -1e30)
            block_max = jnp.max(scores, axis=1, keepdims=True)
            if first:
                new_max = block_max
                weights = jnp.exp2(scores - new_max)
                new_sum = jnp.sum(weights, axis=1, keepdims=True)
            else:
                old_max = max_in[:, columns][:, :1]
                new_max = jnp.maximum(old_max, block_max)
                weights = jnp.exp2(scores - new_max)
                rescale = jnp.exp2(old_max - new_max)
                new_sum = sum_in[:, columns][:, :1] * rescale + jnp.sum(
                    weights, axis=1, keepdims=True
                )
            mixture = jnp.dot(
                weights.astype(jnp.bfloat16), values, preferred_element_type=jnp.float32
            )
            if not first:
                mixture = acc_in[:, columns] * rescale + mixture
            if last:
                outs[0][:, columns] = (mixture / new_sum).astype(jnp.bfloat16)
            else:
                outs[0][:, columns] = mixture
                outs[1][:, columns] = jnp.broadcast_to(new_max, (tile, HEAD_DIM))
                outs[2][:, columns] = jnp.broadcast_to(new_sum, (tile, HEAD_DIM))

    def keep():
        if last:
            for h in range(heads):
                columns = slice(h * HEAD_DIM, (h + 1) * HEAD_DIM)
                outs[0][:, columns] = (acc_in[:, columns] / sum_in[:, columns]).astype(
                    jnp.bfloat16
                )
        elif first:
            outs[0][...] = jnp.zeros_like(outs[0])
            outs[1][...] = jnp.full_like(outs[1], -1e30)
            outs[2][...] = jnp.zeros_like(outs[2])
        else:
            outs[0][...] = acc_in[...]
            outs[1][...] = max_in[...]
            outs[2][...] = sum_in[...]

    needed = info_ref[3] > 0
    if causal:
        needed = jnp.logical_and(needed, key_first <= q_first + (tile - 1))
    pl.when(needed)(lambda: step(None))
    pl.when(jnp.logical_not(needed))(keep)


def flash(info, q, fq, kv, state, *, heads, rows, tile, causal, last, gate_rows):
    total = q.shape[0]
    width = heads * HEAD_DIM
    row_spec = pl.BlockSpec((tile, width), lambda i: (i, 0))
    in_specs = [
        pl.BlockSpec(memory_space=pltpu.SMEM),
        row_spec,
        pl.BlockSpec((None,) + fq.shape[1:], lambda i: (i, 0, 0)),
        pl.BlockSpec(kv.shape, lambda i: (0, 0)),
    ]
    operands = [info, q, fq, kv]
    if state is not None:
        in_specs += [row_spec] * 3
        operands += list(state)
    if last:
        out_shape = jax.ShapeDtypeStruct((total, width), jnp.bfloat16)
        out_specs = row_spec
    else:
        out_shape = [jax.ShapeDtypeStruct((total, width), jnp.float32)] * 3
        out_specs = [row_spec] * 3
    return pl.pallas_call(
        functools.partial(
            flash_body,
            heads=heads,
            rows=rows,
            causal=causal,
            first=state is None,
            last=last,
            gate_rows=gate_rows,
        ),
        grid=(total // tile,),
        in_specs=in_specs,
        out_specs=out_specs,
        out_shape=out_shape,
        compiler_params=pltpu.CompilerParams(
            dimension_semantics=("arbitrary",), vmem_limit_bytes=40 * 1024 * 1024
        ),
        cost_estimate=pl.CostEstimate(
            flops=total * rows * width * 16,
            bytes_accessed=total * width * 24,
            transcendentals=total * rows * heads,
        ),
        name="flash",
    )(*operands)


def on_device(
    inputs,
    w_query,
    w_key,
    w_value,
    w_glu_value,
    w_glu_gate,
    conv_taps,
    conv_gain,
    log_forget,
    w_out,
):
    f32 = jnp.float32
    tok_rows = inputs.shape[0]
    channels = w_glu_value.shape[1]
    heads_here = w_query.shape[1] // HEAD_DIM
    tp_count = lax.axis_size("tp")
    sp_count = lax.axis_size("sp")
    sp_place = lax.axis_index("sp")
    total_channels = channels * tp_count
    out_rows = tok_rows // tp_count
    group = 2 if heads_here % 2 == 0 and sp_count % 2 == 0 else 1
    heads = heads_here // group
    width = heads * HEAD_DIM
    place = lax.rem(sp_place, group)
    block = sp_place // group
    blocks = sp_count // group
    gate_rows = tok_rows // (2 * width)
    pad_rows = -(heads * GATE_PARTS * gate_rows) % 16

    def swap(value):
        return lax.ppermute(value, "sp", [(i, i ^ 1) for i in range(sp_count)])

    def hop(value):
        return lax.ppermute(
            value, "sp", [(i, i + group) for i in range(sp_count - group)]
        )

    def columns_of(array, which, size):
        return lax.dynamic_slice_in_dim(array, which * size, size, 1)

    def keys_and_values(which):
        weight = jnp.concatenate(
            [columns_of(w_key, which, width), columns_of(w_value, which, width)], axis=1
        )
        both = jnp.dot(inputs, weight, preferred_element_type=f32).astype(jnp.bfloat16)
        gates = columns_of(log_forget, which, heads).T
        extra = jnp.swapaxes(split_gates(gates), 0, 1).reshape(-1, 2 * width)
        extra = jnp.pad(extra, ((0, pad_rows), (0, 0)))
        return jnp.concatenate([both, extra], axis=0), gates

    if group == 2:
        kv_send, _ = keys_and_values(1 - place)
        kv_partner = swap(kv_send)
        kv_own, gates_own = keys_and_values(place)
        halves = [kv_own, kv_partner]
    else:
        kv_own, gates_own = keys_and_values(place)
        halves = [kv_own]
    query_rows = jnp.dot(inputs, w_query, preferred_element_type=f32).astype(jnp.bfloat16)
    q = columns_of(query_rows, place, width)
    if group == 2:
        q_partner = swap(columns_of(query_rows, 1 - place, width))
        q = jnp.concatenate([q, q_partner], axis=0)

    glu_value = jnp.dot(inputs, w_glu_value, preferred_element_type=f32)
    glu_gate = jnp.dot(inputs, w_glu_gate, preferred_element_type=f32)
    gated = (glu_value * jax.nn.sigmoid(glu_gate)).astype(jnp.bfloat16)
    kernel = conv_taps.shape[0]
    halo = -(-(kernel - 1) // 16) * 16
    halo_rows = lax.ppermute(
        gated[tok_rows - halo :], "sp", [(i, i + 1) for i in range(sp_count - 1)]
    )
    padded = jnp.concatenate([halo_rows, gated], axis=0)
    windows = jnp.concatenate(
        [padded[t * out_rows : t * out_rows + out_rows + halo] for t in range(tp_count)], axis=0
    )
    windows = lax.all_to_all(windows, "tp", 0, 0, tiled=True).reshape(
        tp_count, out_rows + halo, channels
    )
    parameters = lax.all_gather(
        jnp.concatenate([conv_taps, conv_gain[None]], axis=0), "tp", axis=0
    )
    wide = windows.astype(f32)
    conv_sum = jnp.zeros((tp_count, out_rows, channels), f32)
    for offset in range(kernel):
        start = offset + halo - (kernel - 1)
        conv_sum = conv_sum + parameters[:, offset : offset + 1] * wide[:, start : start + out_rows]
    mean_value = jnp.sum(conv_sum, axis=(0, 2), keepdims=True) / total_channels
    centered = conv_sum - mean_value
    spread = jnp.sum(centered * centered, axis=(0, 2), keepdims=True) / total_channels
    conv_rows = jax.nn.silu(
        centered * lax.rsqrt(spread + NORM_EPS) * parameters[:, kernel : kernel + 1]
    ).astype(jnp.bfloat16)
    conv_rows = jnp.swapaxes(conv_rows, 0, 1).reshape(out_rows, total_channels)
    projected = jnp.dot(conv_rows, w_out[:total_channels], preferred_element_type=f32)

    tile = min(512, tok_rows)
    tiles_half = tok_rows // tile

    def packed_gates(half):
        extra = half[tok_rows : tok_rows + heads * GATE_PARTS * gate_rows].astype(f32)
        return extra.reshape(heads, GATE_PARTS, tok_rows).sum(axis=1)

    fq_parts = [gates_own] + [packed_gates(half) for half in halves[1:]]
    fq = jnp.concatenate(
        [part.reshape(heads, tiles_half, tile)[:, :, 0].T for part in fq_parts], axis=0
    )
    fq = jnp.broadcast_to(fq[:, :, None], fq.shape + (HEAD_DIM,))
    rows_own = place * tok_rows
    rows_partner = (group - 1 - place) * tok_rows
    offsets = [rows_own, rows_partner]

    def run(half, key_first, valid, state, causal, last):
        info = jnp.stack(
            [rows_own, rows_partner - rows_own, key_first, valid]
        ).astype(jnp.int32)
        return flash(
            info,
            q,
            fq,
            half,
            state,
            heads=heads,
            rows=tok_rows,
            tile=tile,
            causal=causal,
            last=last,
            gate_rows=gate_rows,
        )

    state = None
    for number in range(blocks):
        ready = halves
        if number < blocks - 1:
            halves = [hop(half) for half in ready]
        for part, half in enumerate(ready):
            finished = number == blocks - 1 and part == len(ready) - 1
            valid = (block >= number).astype(jnp.int32)
            state = run(half, offsets[part], valid, state, number == 0, finished)
    attn = state
    if group == 2:
        back = swap(attn[tok_rows:])
        mine = attn[:tok_rows]
        first_head = jnp.where(place == 0, mine, back)
        second_head = jnp.where(place == 0, back, mine)
        attn = jnp.concatenate([first_head, second_head], axis=1)
    attn = lax.all_to_all(attn, "tp", 0, 0, tiled=True)
    attn = jnp.swapaxes(attn.reshape(tp_count, out_rows, heads_here * HEAD_DIM), 0, 1)
    attn = attn.reshape(out_rows, tp_count * heads_here * HEAD_DIM)
    return (
        projected + jnp.dot(attn, w_out[total_channels:], preferred_element_type=f32)
    ).astype(jnp.bfloat16)


def solution(mesh):
    in_specs = (
        P("sp", None),
        P(None, "tp"),
        P(None, "tp"),
        P(None, "tp"),
        P(None, "tp"),
        P(None, "tp"),
        P(None, "tp"),
        P("tp"),
        P("sp", "tp"),
        P(),
    )
    out_specs = P(("sp", "tp"), None)
    return jax.shard_map(
        on_device, mesh=mesh, in_specs=in_specs, out_specs=out_specs, check_vma=False
    )
```

```python
import functools

import jax
import jax.numpy as jnp
from jax import lax
from jax.experimental import pallas as pl
from jax.experimental.pallas import tpu as pltpu
from jax.sharding import PartitionSpec as P

HEAD_DIM = 128
NORM_EPS = 1e-05
LOG2E = 1.4426950408889634
GATE_PARTS = 3
SUB_ROWS = 256


def split_gates(gates):
    high = lax.reduce_precision(gates, 8, 7)
    middle = lax.reduce_precision(gates - high, 8, 7)
    low = gates - high - middle
    return jnp.stack([high, middle, low]).astype(jnp.bfloat16)


def flash_body(
    info_ref,
    shift_ref,
    q_ref,
    kv_ref,
    *refs,
    heads,
    rows,
    sub,
    causal,
    first,
    last,
    gate_rows,
):
    if first:
        outs = refs
    else:
        acc_in, max_in, sum_in = refs[:3]
        outs = refs[3:]
    width = heads * HEAD_DIM
    tile = q_ref.shape[0]
    q_first = pl.program_id(0) * tile
    key_first = info_ref[0]

    def step():
        for h in range(heads):
            columns = slice(h * HEAD_DIM, (h + 1) * HEAD_DIM)
            keys = kv_ref[:rows, columns]
            values = kv_ref[:rows, width + h * HEAD_DIM : width + (h + 1) * HEAD_DIM]
            values = jnp.concatenate([values, jnp.ones_like(values)], axis=1)
            base = rows + h * GATE_PARTS * gate_rows
            packed = kv_ref[base : base + GATE_PARTS * gate_rows, :].astype(jnp.float32)
            pieces = []
            for g in range(gate_rows):
                total = packed[g : g + 1]
                for part in range(1, GATE_PARTS):
                    total = total + packed[part * gate_rows + g : part * gate_rows + g + 1]
                pieces.append(total)
            gates = jnp.concatenate(pieces, axis=1)
            bias = (shift_ref[h] - gates) * LOG2E
            for begin in range(0, tile, sub):
                here = slice(begin, begin + sub)
                scores = lax.dot_general(
                    q_ref[here, columns],
                    keys,
                    (((1,), (1,)), ((), ())),
                    preferred_element_type=jnp.float32,
                )
                scores = scores * (HEAD_DIM ** (-0.5) * LOG2E) + bias
                if causal:
                    ahead = q_first + begin - key_first
                    row_pos = ahead + lax.broadcasted_iota(jnp.int32, scores.shape, 0)
                    key_pos = lax.broadcasted_iota(jnp.int32, scores.shape, 1)
                    scores = jnp.where(key_pos <= row_pos, scores, -1e30)
                new_max = jnp.max(scores, axis=1, keepdims=True)
                if not first:
                    old_max = max_in[here, columns][:, :1]
                    new_max = jnp.maximum(old_max, new_max)
                weights = jnp.exp2(scores - new_max).astype(jnp.bfloat16)
                both = jnp.dot(weights, values, preferred_element_type=jnp.float32)
                mixture, new_sum = both[:, :HEAD_DIM], both[:, HEAD_DIM:]
                if not first:
                    rescale = jnp.exp2(old_max - new_max)
                    mixture = acc_in[here, columns] * rescale + mixture
                    new_sum = sum_in[here, columns] * rescale + new_sum
                if last:
                    outs[0][here, columns] = (mixture / new_sum).astype(jnp.bfloat16)
                else:
                    outs[0][here, columns] = mixture
                    outs[1][here, columns] = jnp.broadcast_to(new_max, mixture.shape)
                    outs[2][here, columns] = new_sum

    def keep():
        if last:
            outs[0][...] = (acc_in[...] / sum_in[...]).astype(jnp.bfloat16)
        elif first:
            outs[0][...] = jnp.zeros_like(outs[0])
            outs[1][...] = jnp.full_like(outs[1], -1e30)
            outs[2][...] = jnp.zeros_like(outs[2])
        else:
            outs[0][...] = acc_in[...]
            outs[1][...] = max_in[...]
            outs[2][...] = sum_in[...]

    needed = info_ref[1] > 0
    if causal:
        needed = jnp.logical_and(needed, key_first <= q_first + (tile - 1))
    pl.when(needed)(step)
    pl.when(jnp.logical_not(needed))(keep)


def flash(info, shift, q, kv, state, *, heads, rows, tile, sub, causal, last, gate_rows):
    total = q.shape[0]
    width = heads * HEAD_DIM
    row_spec = pl.BlockSpec((tile, width), lambda i: (i, 0))
    in_specs = [
        pl.BlockSpec(memory_space=pltpu.SMEM),
        pl.BlockSpec(memory_space=pltpu.SMEM),
        row_spec,
        pl.BlockSpec(kv.shape, lambda i: (0, 0)),
    ]
    operands = [info, shift, q, kv]
    if state is not None:
        in_specs += [row_spec] * 3
        operands += list(state)
    if last:
        out_shape = jax.ShapeDtypeStruct((total, width), jnp.bfloat16)
        out_specs = row_spec
    else:
        out_shape = [jax.ShapeDtypeStruct((total, width), jnp.float32)] * 3
        out_specs = [row_spec] * 3
    return pl.pallas_call(
        functools.partial(
            flash_body,
            heads=heads,
            rows=rows,
            sub=sub,
            causal=causal,
            first=state is None,
            last=last,
            gate_rows=gate_rows,
        ),
        grid=(total // tile,),
        in_specs=in_specs,
        out_specs=out_specs,
        out_shape=out_shape,
        compiler_params=pltpu.CompilerParams(
            dimension_semantics=("arbitrary",), vmem_limit_bytes=40 * 1024 * 1024
        ),
        cost_estimate=pl.CostEstimate(
            flops=total * rows * width * 16,
            bytes_accessed=total * width * 24,
            transcendentals=total * rows * heads,
        ),
        name="flash",
    )(*operands)


def conv_body(window_ref, out_ref, sums_ref, *, taps, halo, rows, total_channels):
    groups, _, channels = window_ref.shape
    table = rows + halo
    total = jnp.zeros((rows, 1), jnp.float32)
    for g in range(groups):
        parts = window_ref[g, table:, :].astype(jnp.float32)
        count = parts.shape[0] // GATE_PARTS
        weights = parts[:count] + parts[count : 2 * count] + parts[2 * count :]
        sums_ref[g, 0, :table, :] = window_ref[g, :table, :].astype(jnp.float32)
        sums_ref[g, 1, :count, :] = weights
    for g in range(groups):
        for c in range(0, channels, HEAD_DIM):
            lanes = slice(c, c + HEAD_DIM)
            acc = jnp.zeros((rows, HEAD_DIM), jnp.float32)
            for offset in range(taps):
                start = offset + halo - (taps - 1)
                acc = acc + sums_ref[g, 1, offset : offset + 1, lanes] * (
                    sums_ref[g, 0, start : start + rows, lanes]
                )
            total = total + jnp.sum(acc, axis=1, keepdims=True)
            sums_ref[g, 2, :rows, lanes] = acc
    mean_value = total / total_channels
    squares = jnp.zeros((rows, 1), jnp.float32)
    for g in range(groups):
        centered = sums_ref[g, 2, :rows, :] - mean_value
        squares = squares + jnp.sum(centered * centered, axis=1, keepdims=True)
    factor = lax.rsqrt(squares / total_channels + NORM_EPS)
    for g in range(groups):
        centered = sums_ref[g, 2, :rows, :] - mean_value
        values = centered * factor * sums_ref[g, 1, taps : taps + 1, :]
        out_ref[:, g * channels : (g + 1) * channels] = (
            values / (1.0 + jnp.exp(-values))
        ).astype(jnp.bfloat16)


def convolve(windows, *, taps, halo, rows, total_channels):
    groups, depth, channels = windows.shape
    return pl.pallas_call(
        functools.partial(
            conv_body, taps=taps, halo=halo, rows=rows, total_channels=total_channels
        ),
        out_shape=jax.ShapeDtypeStruct((rows, total_channels), jnp.bfloat16),
        scratch_shapes=[pltpu.VMEM((groups, 3, rows + halo, channels), jnp.float32)],
        compiler_params=pltpu.CompilerParams(vmem_limit_bytes=40 * 1024 * 1024),
        cost_estimate=pl.CostEstimate(
            flops=total_channels * rows * taps * 64, bytes_accessed=1 << 21, transcendentals=0
        ),
        name="convolve",
    )(windows)


def on_device(
    inputs,
    w_query,
    w_key,
    w_value,
    w_glu_value,
    w_glu_gate,
    conv_taps,
    conv_gain,
    log_forget,
    w_out,
):
    f32 = jnp.float32
    tok_rows = inputs.shape[0]
    channels = w_glu_value.shape[1]
    heads_here = w_query.shape[1] // HEAD_DIM
    tp_count = lax.axis_size("tp")
    sp_count = lax.axis_size("sp")
    sp_place = lax.axis_index("sp")
    total_channels = channels * tp_count
    out_rows = tok_rows // tp_count
    group = 2 if heads_here % 2 == 0 and sp_count % 2 == 0 else 1
    heads = heads_here // group
    width = heads * HEAD_DIM
    place = lax.rem(sp_place, group)
    block = sp_place // group
    blocks = sp_count // group
    gate_rows = tok_rows // (2 * width)
    pad_rows = -(heads * GATE_PARTS * gate_rows) % 16

    def swap(value):
        return lax.ppermute(value, "sp", [(i, i ^ 1) for i in range(sp_count)])

    def hop(value):
        return lax.ppermute(
            value, "sp", [(i, i + group) for i in range(sp_count - group)]
        )

    def columns_of(array, which, size):
        return lax.dynamic_slice_in_dim(array, which * size, size, 1)

    def keys_and_values(which):
        weight = jnp.concatenate(
            [columns_of(w_key, which, width), columns_of(w_value, which, width)], axis=1
        )
        both = jnp.dot(inputs, weight, preferred_element_type=f32).astype(jnp.bfloat16)
        gates = columns_of(log_forget, which, heads).T
        extra = jnp.swapaxes(split_gates(gates), 0, 1).reshape(-1, 2 * width)
        extra = jnp.pad(extra, ((0, pad_rows), (0, 0)))
        return jnp.concatenate([both, extra], axis=0), gates

    if group == 2:
        kv_send, _ = keys_and_values(1 - place)
        kv_partner = swap(kv_send)
        kv_own, gates_own = keys_and_values(place)
        halves = [kv_own, kv_partner]
    else:
        kv_own, gates_own = keys_and_values(place)
        halves = [kv_own]
    query_rows = jnp.dot(inputs, w_query, preferred_element_type=f32).astype(jnp.bfloat16)
    q = columns_of(query_rows, place, width)
    if group == 2:
        q_partner = swap(columns_of(query_rows, 1 - place, width))
        q = jnp.where(
            place == 0,
            jnp.concatenate([q, q_partner], axis=0),
            jnp.concatenate([q_partner, q], axis=0),
        )

    glu_value = jnp.dot(inputs, w_glu_value, preferred_element_type=f32)
    glu_gate = jnp.dot(inputs, w_glu_gate, preferred_element_type=f32)
    gated = (glu_value * jax.nn.sigmoid(glu_gate)).astype(jnp.bfloat16)
    kernel = conv_taps.shape[0]
    halo = -(-(kernel - 1) // 16) * 16
    halo_rows = lax.ppermute(
        gated[tok_rows - halo :], "sp", [(i, i + 1) for i in range(sp_count - 1)]
    )
    padded = jnp.concatenate([halo_rows, gated], axis=0)
    table = split_gates(jnp.concatenate([conv_taps, conv_gain[None]], axis=0))
    table = table.reshape(-1, channels)
    pieces = []
    for t in range(tp_count):
        pieces += [padded[t * out_rows : t * out_rows + out_rows + halo], table]
    windows = lax.all_to_all(jnp.concatenate(pieces, axis=0), "tp", 0, 0, tiled=True)
    windows = windows.reshape(tp_count, -1, channels)

    tile = min(512, tok_rows)
    shift = gates_own[:, 0]
    offsets = [place * tok_rows, (group - 1 - place) * tok_rows]

    def run(half, key_first, valid, state, causal, last):
        info = jnp.stack([key_first, valid]).astype(jnp.int32)
        return flash(
            info,
            shift,
            q,
            half,
            state,
            heads=heads,
            rows=tok_rows,
            tile=tile,
            sub=min(SUB_ROWS, tile),
            causal=causal,
            last=last,
            gate_rows=gate_rows,
        )

    state = None
    for number in range(blocks):
        ready = halves
        if number < blocks - 1:
            halves = [hop(half) for half in ready]
        for part, half in enumerate(ready):
            finished = number == blocks - 1 and part == len(ready) - 1
            valid = (block >= number).astype(jnp.int32)
            state = run(half, offsets[part], valid, state, number == 0, finished)
    windows, attn = lax.optimization_barrier((windows, state))
    if group == 2:
        members = [
            [
                (base + r) * tp_count + t
                for r in range(group)
                for t in range(tp_count)
            ]
            for base in range(0, sp_count, group)
        ]
        attn = lax.all_to_all(
            attn, ("sp", "tp"), 0, 0, axis_index_groups=members, tiled=True
        )
        attn = attn.reshape(group, tp_count, out_rows, width)
    else:
        attn = lax.all_to_all(attn, "tp", 0, 0, tiled=True)
        attn = attn.reshape(1, tp_count, out_rows, width)
    conv_rows = convolve(
        windows, taps=kernel, halo=halo, rows=out_rows, total_channels=total_channels
    )
    projected = jnp.dot(conv_rows, w_out[:total_channels], preferred_element_type=f32)
    attn = jnp.transpose(attn, (2, 1, 0, 3)).reshape(out_rows, -1)
    return (
        projected + jnp.dot(attn, w_out[total_channels:], preferred_element_type=f32)
    ).astype(jnp.bfloat16)


def solution(mesh):
    in_specs = (
        P("sp", None),
        P(None, "tp"),
        P(None, "tp"),
        P(None, "tp"),
        P(None, "tp"),
        P(None, "tp"),
        P(None, "tp"),
        P("tp"),
        P("sp", "tp"),
        P(),
    )
    out_specs = P(("sp", "tp"), None)
    return jax.shard_map(
        on_device, mesh=mesh, in_specs=in_specs, out_specs=out_specs, check_vma=False
    )
```

```python
import functools

import jax
import jax.numpy as jnp
from jax import lax
from jax.experimental import pallas as pl
from jax.experimental.pallas import tpu as pltpu
from jax.sharding import PartitionSpec as P

HEAD_DIM = 128
NORM_EPS = 1e-05
LOG2E = 1.4426950408889634
GATE_PARTS = 3
SUB_ROWS = 256


def split_gates(gates):
    high = lax.reduce_precision(gates, 8, 7)
    middle = lax.reduce_precision(gates - high, 8, 7)
    low = gates - high - middle
    return jnp.stack([high, middle, low]).astype(jnp.bfloat16)


def flash_body(
    info_ref,
    shift_ref,
    q_ref,
    kv_ref,
    *refs,
    heads,
    rows,
    sub,
    causal,
    first,
    last,
    gate_rows,
):
    if first:
        outs = refs
    else:
        acc_in, max_in, sum_in = refs[:3]
        outs = refs[3:]
    width = heads * HEAD_DIM
    tile = q_ref.shape[0]
    q_first = pl.program_id(0) * tile
    key_first = info_ref[0]

    def step():
        for h in range(heads):
            columns = slice(h * HEAD_DIM, (h + 1) * HEAD_DIM)
            keys = kv_ref[:rows, columns]
            values = kv_ref[:rows, width + h * HEAD_DIM : width + (h + 1) * HEAD_DIM]
            values = jnp.concatenate([values, jnp.ones_like(values)], axis=1)
            base = rows + h * GATE_PARTS * gate_rows
            packed = kv_ref[base : base + GATE_PARTS * gate_rows, :].astype(jnp.float32)
            pieces = []
            for g in range(gate_rows):
                total = packed[g : g + 1]
                for part in range(1, GATE_PARTS):
                    total = total + packed[part * gate_rows + g : part * gate_rows + g + 1]
                pieces.append(total)
            gates = jnp.concatenate(pieces, axis=1)
            bias = (shift_ref[h] - gates) * LOG2E
            for begin in range(0, tile, sub):
                here = slice(begin, begin + sub)
                scores = lax.dot_general(
                    q_ref[here, columns],
                    keys,
                    (((1,), (1,)), ((), ())),
                    preferred_element_type=jnp.float32,
                )
                scores = scores * (HEAD_DIM ** (-0.5) * LOG2E) + bias
                if causal:
                    ahead = q_first + begin - key_first
                    row_pos = ahead + lax.broadcasted_iota(jnp.int32, scores.shape, 0)
                    key_pos = lax.broadcasted_iota(jnp.int32, scores.shape, 1)
                    scores = jnp.where(key_pos <= row_pos, scores, -1e30)
                new_max = jnp.max(scores, axis=1, keepdims=True)
                if not first:
                    old_max = max_in[here, columns][:, :1]
                    new_max = jnp.maximum(old_max, new_max)
                weights = jnp.exp2(scores - new_max).astype(jnp.bfloat16)
                both = jnp.dot(weights, values, preferred_element_type=jnp.float32)
                mixture, new_sum = both[:, :HEAD_DIM], both[:, HEAD_DIM:]
                if not first:
                    rescale = jnp.exp2(old_max - new_max)
                    mixture = acc_in[here, columns] * rescale + mixture
                    new_sum = sum_in[here, columns] * rescale + new_sum
                if last:
                    outs[0][here, columns] = (mixture / new_sum).astype(jnp.bfloat16)
                else:
                    outs[0][here, columns] = mixture
                    outs[1][here, columns] = jnp.broadcast_to(new_max, mixture.shape)
                    outs[2][here, columns] = new_sum

    def keep():
        if last:
            outs[0][...] = (acc_in[...] / sum_in[...]).astype(jnp.bfloat16)
        elif first:
            outs[0][...] = jnp.zeros_like(outs[0])
            outs[1][...] = jnp.full_like(outs[1], -1e30)
            outs[2][...] = jnp.zeros_like(outs[2])
        else:
            outs[0][...] = acc_in[...]
            outs[1][...] = max_in[...]
            outs[2][...] = sum_in[...]

    needed = info_ref[1] > 0
    if causal:
        needed = jnp.logical_and(needed, key_first <= q_first + (tile - 1))
    pl.when(needed)(step)
    pl.when(jnp.logical_not(needed))(keep)


def flash(info, shift, q, kv, state, *, heads, rows, tile, sub, causal, last, gate_rows):
    total = q.shape[0]
    width = heads * HEAD_DIM
    row_spec = pl.BlockSpec((tile, width), lambda i: (i, 0))
    in_specs = [
        pl.BlockSpec(memory_space=pltpu.SMEM),
        pl.BlockSpec(memory_space=pltpu.SMEM),
        row_spec,
        pl.BlockSpec(kv.shape, lambda i: (0, 0)),
    ]
    operands = [info, shift, q, kv]
    if state is not None:
        in_specs += [row_spec] * 3
        operands += list(state)
    if last:
        out_shape = jax.ShapeDtypeStruct((total, width), jnp.bfloat16)
        out_specs = row_spec
    else:
        out_shape = [jax.ShapeDtypeStruct((total, width), jnp.float32)] * 3
        out_specs = [row_spec] * 3
    return pl.pallas_call(
        functools.partial(
            flash_body,
            heads=heads,
            rows=rows,
            sub=sub,
            causal=causal,
            first=state is None,
            last=last,
            gate_rows=gate_rows,
        ),
        grid=(total // tile,),
        in_specs=in_specs,
        out_specs=out_specs,
        out_shape=out_shape,
        compiler_params=pltpu.CompilerParams(
            dimension_semantics=("arbitrary",), vmem_limit_bytes=40 * 1024 * 1024
        ),
        cost_estimate=pl.CostEstimate(
            flops=total * rows * width * 16,
            bytes_accessed=total * width * 24,
            transcendentals=total * rows * heads,
        ),
        name="flash",
    )(*operands)


def conv_body(window_ref, out_ref, sums_ref, *, taps, halo, rows, total_channels):
    groups, _, channels = window_ref.shape
    table = rows + halo
    total = jnp.zeros((rows, 1), jnp.float32)
    for g in range(groups):
        parts = window_ref[g, table:, :].astype(jnp.float32)
        count = parts.shape[0] // GATE_PARTS
        weights = parts[:count] + parts[count : 2 * count] + parts[2 * count :]
        sums_ref[g, 0, :table, :] = window_ref[g, :table, :].astype(jnp.float32)
        sums_ref[g, 1, :count, :] = weights
    for g in range(groups):
        for c in range(0, channels, HEAD_DIM):
            lanes = slice(c, c + HEAD_DIM)
            acc = jnp.zeros((rows, HEAD_DIM), jnp.float32)
            for offset in range(taps):
                start = offset + halo - (taps - 1)
                acc = acc + sums_ref[g, 1, offset : offset + 1, lanes] * (
                    sums_ref[g, 0, start : start + rows, lanes]
                )
            total = total + jnp.sum(acc, axis=1, keepdims=True)
            sums_ref[g, 2, :rows, lanes] = acc
    mean_value = total / total_channels
    squares = jnp.zeros((rows, 1), jnp.float32)
    for g in range(groups):
        centered = sums_ref[g, 2, :rows, :] - mean_value
        squares = squares + jnp.sum(centered * centered, axis=1, keepdims=True)
    factor = lax.rsqrt(squares / total_channels + NORM_EPS)
    for g in range(groups):
        centered = sums_ref[g, 2, :rows, :] - mean_value
        values = centered * factor * sums_ref[g, 1, taps : taps + 1, :]
        out_ref[:, g * channels : (g + 1) * channels] = (
            values / (1.0 + jnp.exp(-values))
        ).astype(jnp.bfloat16)


def convolve(windows, *, taps, halo, rows, total_channels):
    groups, _, channels = windows.shape
    return pl.pallas_call(
        functools.partial(
            conv_body, taps=taps, halo=halo, rows=rows, total_channels=total_channels
        ),
        out_shape=jax.ShapeDtypeStruct((rows, total_channels), jnp.bfloat16),
        scratch_shapes=[pltpu.VMEM((groups, 3, rows + halo, channels), jnp.float32)],
        compiler_params=pltpu.CompilerParams(vmem_limit_bytes=40 * 1024 * 1024),
        cost_estimate=pl.CostEstimate(
            flops=total_channels * rows * taps * 64, bytes_accessed=1 << 21, transcendentals=0
        ),
        name="convolve",
    )(windows)


def layer(
    inputs,
    w_query,
    w_key,
    w_value,
    w_glu_value,
    w_glu_gate,
    conv_taps,
    conv_gain,
    log_forget,
    w_out,
):
    f32 = jnp.float32
    tok_rows = inputs.shape[0]
    channels = w_glu_value.shape[1]
    heads_here = w_query.shape[1] // HEAD_DIM
    tp_count = lax.axis_size("tp")
    sp_count = lax.axis_size("sp")
    sp_place = lax.axis_index("sp")
    total_channels = channels * tp_count
    out_rows = tok_rows // tp_count
    group = 2 if heads_here % 2 == 0 and sp_count % 2 == 0 else 1
    heads = heads_here // group
    width = heads * HEAD_DIM
    place = lax.rem(sp_place, group)
    block = sp_place // group
    blocks = sp_count // group
    gate_rows = tok_rows // (2 * width)
    pad_rows = -(heads * GATE_PARTS * gate_rows) % 16

    def swap(value):
        return lax.ppermute(value, "sp", [(i, i ^ 1) for i in range(sp_count)])

    def hop(value):
        return lax.ppermute(
            value, "sp", [(i, i + group) for i in range(sp_count - group)]
        )

    def columns_of(array, which, size):
        return lax.dynamic_slice_in_dim(array, which * size, size, 1)

    def keys_and_values(which):
        weight = jnp.concatenate(
            [columns_of(w_key, which, width), columns_of(w_value, which, width)], axis=1
        )
        both = jnp.dot(inputs, weight, preferred_element_type=f32).astype(jnp.bfloat16)
        gates = columns_of(log_forget, which, heads).T
        extra = jnp.swapaxes(split_gates(gates), 0, 1).reshape(-1, 2 * width)
        extra = jnp.pad(extra, ((0, pad_rows), (0, 0)))
        return jnp.concatenate([both, extra], axis=0), gates

    if group == 2:
        kv_send, _ = keys_and_values(1 - place)
        kv_partner = swap(kv_send)
        kv_own, gates_own = keys_and_values(place)
        halves = [kv_own, kv_partner]
    else:
        kv_own, gates_own = keys_and_values(place)
        halves = [kv_own]
    inputs, kv_own = lax.optimization_barrier((inputs, kv_own))
    halves[0] = kv_own
    query_rows = jnp.dot(inputs, w_query, preferred_element_type=f32).astype(jnp.bfloat16)
    q = columns_of(query_rows, place, width)
    if group == 2:
        q_other = columns_of(query_rows, 1 - place, width)
        q_partner = swap(q_other)
        q = jnp.where(
            place == 0,
            jnp.concatenate([q, q_partner], axis=0),
            jnp.concatenate([q_partner, q], axis=0),
        )

    glu_value = jnp.dot(inputs, w_glu_value, preferred_element_type=f32)
    glu_gate = jnp.dot(inputs, w_glu_gate, preferred_element_type=f32)
    gated = (glu_value * jax.nn.sigmoid(glu_gate)).astype(jnp.bfloat16)
    kernel = conv_taps.shape[0]
    halo = -(-(kernel - 1) // 16) * 16
    halo_rows = lax.ppermute(
        gated[tok_rows - halo :], "sp", [(i, i + 1) for i in range(sp_count - 1)]
    )
    padded = jnp.concatenate([halo_rows, gated], axis=0)
    table = split_gates(jnp.concatenate([conv_taps, conv_gain[None]], axis=0))
    table = table.reshape(-1, channels)
    pieces = []
    for t in range(tp_count):
        pieces += [padded[t * out_rows : t * out_rows + out_rows + halo], table]
    pieces = jnp.concatenate(pieces, axis=0)
    windows = lax.all_to_all(pieces, "tp", 0, 0, tiled=True)
    windows = windows.reshape(tp_count, -1, channels)

    tile = min(512, tok_rows)
    shift = gates_own[:, 0]
    offsets = [place * tok_rows, (group - 1 - place) * tok_rows]

    def run(half, key_first, valid, state, causal, last):
        info = jnp.stack([key_first, valid]).astype(jnp.int32)
        return flash(
            info,
            shift,
            q,
            half,
            state,
            heads=heads,
            rows=tok_rows,
            tile=tile,
            sub=min(SUB_ROWS, tile),
            causal=causal,
            last=last,
            gate_rows=gate_rows,
        )

    state = None
    for number in range(blocks):
        ready = halves
        if number < blocks - 1:
            halves = []
            for half in ready:
                halves.append(hop(half))
        for part, half in enumerate(ready):
            finished = number == blocks - 1 and part == len(ready) - 1
            valid = (block >= number).astype(jnp.int32)
            state = run(half, offsets[part], valid, state, number == 0, finished)
    windows, attn = lax.optimization_barrier((windows, state))
    if group == 2:
        members = [
            [
                (base + r) * tp_count + t
                for r in range(group)
                for t in range(tp_count)
            ]
            for base in range(0, sp_count, group)
        ]
        attn = lax.all_to_all(
            attn, ("sp", "tp"), 0, 0, axis_index_groups=members, tiled=True
        )
        attn = attn.reshape(group, tp_count, out_rows, width)
    else:
        attn = lax.all_to_all(attn, "tp", 0, 0, tiled=True)
        attn = attn.reshape(1, tp_count, out_rows, width)
    conv_rows = convolve(
        windows, taps=kernel, halo=halo, rows=out_rows, total_channels=total_channels
    )
    attn = jnp.transpose(attn, (2, 1, 0, 3)).reshape(out_rows, -1)
    both = jnp.concatenate([conv_rows, attn], axis=1)
    return jnp.dot(both, w_out, preferred_element_type=f32).astype(jnp.bfloat16)


def solution(mesh):
    in_specs = (
        P("sp", None),
        P(None, "tp"),
        P(None, "tp"),
        P(None, "tp"),
        P(None, "tp"),
        P(None, "tp"),
        P(None, "tp"),
        P("tp"),
        P("sp", "tp"),
        P(),
    )
    out_specs = P(("sp", "tp"), None)
    return jax.shard_map(
        layer, mesh=mesh, in_specs=in_specs, out_specs=out_specs, check_vma=False
    )
```
